128 devices in a mesh: kv: 16 (over z, y), tp: 8 (over x, core).
Axes of the slice: x: 4, y: 4, z: 4, core: 2. Of those that a mesh axis runs over, the one named last changes fastest.
Arguments:
- activations: bfloat16 [128, 4096], P(None, ('kv', 'tp')), may hold values from -60 to 60
- mixer_gain: bfloat16 [4096], P(('kv', 'tp')), may hold values from 0.099609375 to 1.8984375
- channel_gain: bfloat16 [4096], P(('kv', 'tp')), may hold values from 0.099609375 to 1.8984375
- query_weight: bfloat16 [4096, 4096], P('kv', 'tp'), may hold values from -0.09375 to 0.09375
- key_weight: bfloat16 [4096, 4096], P('kv', 'tp'), may hold values from -0.09375 to 0.09375
- value_weight: bfloat16 [4096, 8192], P('kv', 'tp'), may hold values from -0.09375 to 0.09375
- gate_weight: bfloat16 [4096, 8192], P('kv', 'tp'), may hold values from -0.09375 to 0.09375
- output_weight: bfloat16 [8192, 4096], P('tp', 'kv'), may hold values from -0.1875 to 0.1875
- up_weight: bfloat16 [4096, 16384], P('kv', 'tp'), may hold values from -0.09375 to 0.09375
- down_weight: bfloat16 [16384, 4096], P('tp', 'kv'), may hold values from -0.046875 to 0.046875
- state_in: float32 [128, 16, 256, 512], P('kv', 'tp'), may hold values from -0.5 to 0.5
Outputs:
- activations_out: bfloat16 [128, 4096], P(None, ('kv', 'tp'))
- state_out: float32 [128, 16, 256, 512], P('kv', 'tp')
The draws below stay inside these ranges and needn't reach their ends.
All inputs are finite; a program needn't handle non-finite values.
Results may differ from the reference program's by a relative error of at most 0.022.
Values may be sent and summed in bfloat16 or wider, within the bound.
A program may use at most 64 MiB of HBM per device.

```python
import jax
import jax.numpy as jnp
from jax import lax

D = 4096
HEADS = 16
DK = 256
DV = 512
FF = 16384
BATCH = 128
QK = 4096
RV = 8192
N_TP = 8


def draw_activations(key, part):
    base_key, row_key = jax.random.split(key, 2)
    columns = jnp.exp(jnp.linspace(0.0, jnp.log(3.0), D, dtype=jnp.float32))
    base = jnp.clip(jax.random.normal(base_key, (BATCH, D), jnp.float32), -5.0, 5.0)
    scales = jnp.exp(jax.random.uniform(row_key, (BATCH, 1), jnp.float32, jnp.log(0.3), jnp.log(3.0)))
    return jnp.clip(base * scales * columns, -60.0, 60.0).astype(jnp.bfloat16)


def level_of(key, extent, shards, least, high):
    factor_of, own = 1.0, jax.random.fold_in(key, 6)
    for axis_at, shards_of in shards:
        heights = jnp.exp(jax.random.uniform(jax.random.fold_in(own, axis_at), (shards_of,), jnp.float32, least / len(shards), high / len(shards)))
        factor_of = factor_of * jnp.repeat(heights, extent[axis_at] // shards_of).reshape([-1 if axis == axis_at else 1 for axis in range(len(extent))])
    return factor_of


def normal_values(own_key, dims, spread, most, pieces=(), kind=jnp.bfloat16):
    values = spread * jax.random.normal(own_key, dims, jnp.float32)
    if pieces:
        values = values * level_of(own_key, dims, pieces, -0.22, 0.18)
    return jnp.clip(values, -most, most).astype(kind)


def setup_inputs(seed: int = 0) -> dict:
    key_list = jax.random.split(jax.random.key(seed), 12)
    activations = draw_activations(jax.random.fold_in(key_list[11], 71), 0)
    mixer_gain = jnp.clip(1.0 + 0.18 * jax.random.normal(key_list[1], (D,), jnp.float32), 0.099609375, 1.8984375).astype(jnp.bfloat16)
    channel_gain = jnp.clip(1.0 + 0.18 * jax.random.normal(key_list[2], (D,), jnp.float32), 0.099609375, 1.8984375).astype(jnp.bfloat16)
    query_weight = normal_values(key_list[3], (D, QK), D ** -0.5, 0.09375, ((0, 16), (1, 8)))
    key_weight = normal_values(key_list[4], (D, QK), D ** -0.5, 0.09375, ((0, 16), (1, 8)))
    value_weight = normal_values(key_list[5], (D, RV), D ** -0.5, 0.09375, ((0, 16), (1, 8)))
    gate_weight = normal_values(key_list[6], (D, RV), D ** -0.5, 0.09375, ((0, 16), (1, 8)))
    output_weight = normal_values(key_list[7], (RV, D), (RV // 8) ** -0.5, 0.1875, ((0, 8), (1, 16)))
    up_weight = normal_values(key_list[8], (D, FF), D ** -0.5, 0.09375, ((0, 16), (1, 8)))
    down_weight = normal_values(key_list[9], (FF, D), FF ** -0.5, 0.046875, ((0, 8), (1, 16)))
    state_in = normal_values(key_list[10], (BATCH, HEADS, DK, DV), 0.06, 0.5, ((0, 16), (1, 8)), jnp.float32)
    return dict(activations=activations, mixer_gain=mixer_gain, channel_gain=channel_gain, query_weight=query_weight, key_weight=key_weight, value_weight=value_weight, gate_weight=gate_weight, output_weight=output_weight, up_weight=up_weight, down_weight=down_weight, state_in=state_in)


EPS = 1e-06

def head_decays(count):
    index = jnp.arange(count, dtype=jnp.float32)
    return 1.0 - 2.0 ** (-1.0 - 6.0 * index / (count - 1))

def summed_blocks(left, right, parts):
    width = left.shape[1] // parts
    total = jnp.zeros((left.shape[0], right.shape[1]), jnp.float32)
    for index in range(parts):
        term = jnp.dot(left[:, index * width:(index + 1) * width], right[index * width:(index + 1) * width], preferred_element_type=jnp.float32)
        total = total + lax.optimization_barrier(term.astype(jnp.bfloat16)).astype(jnp.float32)
    return total

def reference(activations, mixer_gain, channel_gain, query_weight, key_weight, value_weight, gate_weight, output_weight, up_weight, down_weight, state_in):
    stream = activations.astype(jnp.float32)
    scale_rows = lax.rsqrt(lax.optimization_barrier(jnp.sum(stream * stream, axis=1, keepdims=True)) / D + EPS)
    normed = (stream * mixer_gain.astype(jnp.float32)).astype(jnp.bfloat16)
    query = scale_rows * jnp.dot(normed, query_weight, preferred_element_type=jnp.float32)
    key = scale_rows * jnp.dot(normed, key_weight, preferred_element_type=jnp.float32) * DK ** (-0.5)
    value = scale_rows * jnp.dot(normed, value_weight, preferred_element_type=jnp.float32)
    gate = scale_rows * jnp.dot(normed, gate_weight, preferred_element_type=jnp.float32)
    rates = head_decays(HEADS)

    def advance(inputs):
        query_row, key_row, value_row, old_state = inputs
        query_heads = query_row.reshape(HEADS, DK)
        key_heads = key_row.reshape(HEADS, DK)
        value_heads = value_row.reshape(HEADS, DV)
        new_state = rates[:, None, None] * old_state + key_heads[:, :, None] * value_heads[:, None, :]
        output = jnp.einsum('hd,hde->he', query_heads, new_state, precision=lax.Precision.HIGHEST)
        return (new_state, output)
    state_out, retained = lax.map(advance, (query, key, value, state_in))
    retained = retained * lax.rsqrt(lax.optimization_barrier(jnp.mean(retained * retained, axis=2, keepdims=True)) + EPS)
    mixed = (jax.nn.silu(gate) * retained.reshape(retained.shape[0], HEADS * DV)).astype(jnp.bfloat16)
    attention = summed_blocks(mixed, output_weight, N_TP)
    middle = (stream + attention).astype(jnp.bfloat16)
    middle = lax.optimization_barrier(middle).astype(jnp.float32)
    channel_scale = lax.rsqrt(lax.optimization_barrier(jnp.sum(middle * middle, axis=1, keepdims=True)) / D + EPS)
    channel_normed = (middle * channel_gain.astype(jnp.float32)).astype(jnp.bfloat16)
    lifted = channel_scale * jnp.dot(channel_normed, up_weight, preferred_element_type=jnp.float32)
    hidden = jnp.square(jax.nn.relu(lifted)).astype(jnp.bfloat16)
    lowered = summed_blocks(hidden, down_weight, N_TP)
    return ((middle + lowered).astype(jnp.bfloat16), state_out)
```

```python
import functools

import jax
import jax.numpy as jnp
from jax import lax
from jax.experimental import pallas as pl
from jax.experimental.pallas import tpu as pltpu
from jax.sharding import PartitionSpec as P

D = 4096
HEADS = 16
DK = 256
DV = 512
EPS = 1e-06
KV = 16
TP = 8
ROWS = 8
HPD = 2
F32 = jnp.float32
BF16 = jnp.bfloat16
MESH = pl.DeviceIdType.MESH


def start_all(axis, n, me, source, dest, send, recv):
    for d in range(1, n):
        peer = lax.rem(me + d, n)
        pltpu.make_async_remote_copy(
            src_ref=source(peer),
            dst_ref=dest.at[me],
            send_sem=send.at[d],
            recv_sem=recv.at[d],
            device_id={axis: peer},
            device_id_type=MESH,
        ).start()


def wait_all(axis, n, me, source, dest, send, recv, which):
    for d in range(1, n):
        peer = lax.rem(me + n - d, n) if which == "recv" else lax.rem(me + d, n)
        copy = pltpu.make_async_remote_copy(
            src_ref=source(peer),
            dst_ref=dest.at[peer],
            send_sem=send.at[d],
            recv_sem=recv.at[d],
            device_id={axis: peer},
            device_id_type=MESH,
        )
        if which == "recv":
            copy.wait_recv()
        else:
            copy.wait_send()


def total(ref, n):
    acc = ref[0].astype(F32)
    for j in range(1, n):
        acc = acc + ref[j].astype(F32)
    return acc


def kernel(
    x_ref, gains_ref, wq_ref, wk_ref, wv_ref, wg_ref, wo_ref, wu_ref, wd_ref, state_ref,
    out_ref, state_out_ref,
    wq, wk, wv, wg, wo, wu, wd, st,
    s1, r1, sa, ra, sv, rv, sg, rg, r4, s5, r5, r6,
    sb0, rb0, sb1, rb1, s7, r7, s8, r8,
    xrows, qt, kt, ret, midt,
    lsem, ss1, rs1, ssa, rsa, ssv, rsv, ssg, rsg, ss4, rs4, ss5, rs5, ss6, rs6,
    ssb0, rsb0, ssb1, rsb1, ss7, rs7, ss8, rs8,
):
    kv = lax.axis_index("kv")
    tp = lax.axis_index("tp")
    barrier = pltpu.get_barrier_semaphore()
    for d in range(1, TP):
        pl.semaphore_signal(barrier, inc=1, device_id={"tp": lax.rem(tp + d, TP)}, device_id_type=MESH)
    for d in range(1, KV):
        pl.semaphore_signal(barrier, inc=1, device_id={"kv": lax.rem(kv + d, KV)}, device_id_type=MESH)
    local = [
        pltpu.make_async_copy(a, b, lsem.at[i])
        for i, (a, b) in enumerate(
            ((wq_ref, wq), (wk_ref, wk), (wv_ref, wv), (wg_ref, wg), (state_ref, st),
             (wo_ref, wo), (wu_ref, wu), (wd_ref, wd))
        )
    ]
    for c in local:
        c.start()

    s1[0:32, :] = jnp.transpose(x_ref[...].astype(F32)).astype(BF16)
    lane = lax.broadcasted_iota(jnp.int32, (16, 128), 1)
    s1[32:48, :] = jnp.where(lane // 32 == lax.rem(tp, 4), gains_ref[...].astype(F32), 0.0).astype(BF16)
    r1[tp] = s1[...]
    pl.semaphore_wait(barrier, TP - 1 + KV - 1)

    one = lambda peer: s1
    start_all("tp", TP, tp, one, r1, ss1, rs1)
    wait_all("tp", TP, tp, one, r1, ss1, rs1, "recv")
    xt = jnp.concatenate([r1[j, 0:32, :].astype(F32) for j in range(TP)], axis=0)
    x = jnp.transpose(xt)
    xrows[...] = x
    halves = [sum(r1[j, 32:48, :].astype(F32) for j in range(4 * i, 4 * i + 4)) for i in range(2)]
    gains = jnp.concatenate(halves, axis=1)
    normed = (x * gains[0:1, :]).astype(BF16)
    squares = jnp.sum(x * x, axis=1, keepdims=True)

    for c in local[:2]:
        c.wait()
    sa[:, :, 0:512] = jnp.dot(normed, wq[...], preferred_element_type=F32).astype(BF16).reshape(KV, ROWS, 512)
    sa[:, :, 512:1024] = jnp.dot(normed, wk[...], preferred_element_type=F32).astype(BF16).reshape(KV, ROWS, 512)
    sa[:, :, 1024:1152] = jnp.broadcast_to(squares, (128, 128)).astype(BF16).reshape(KV, ROWS, 128)
    start_all("kv", KV, kv, lambda peer: sa.at[peer], ra, ssa, rsa)
    local[2].wait()
    sv[...] = jnp.dot(normed, wv[...], preferred_element_type=F32).astype(BF16).reshape(KV, ROWS, 1024)
    start_all("kv", KV, kv, lambda peer: sv.at[peer], rv, ssv, rsv)
    local[3].wait()
    sg[...] = jnp.dot(normed, wg[...], preferred_element_type=F32).astype(BF16).reshape(KV, ROWS, 1024)
    start_all("kv", KV, kv, lambda peer: sg.at[peer], rg, ssg, rsg)
    ra[kv] = sa[kv]
    rv[kv] = sv[kv]
    rg[kv] = sg[kv]

    wait_all("kv", KV, kv, lambda peer: sa.at[peer], ra, ssa, rsa, "recv")
    sums = total(ra, KV)
    scale = lax.rsqrt(sums[:, 1024:1025] / D + EPS)
    query = scale * sums[:, 0:512]
    key = scale * sums[:, 512:1024] * DK ** (-0.5)
    qt[...] = jnp.transpose(query)
    kt[...] = jnp.transpose(key)
    local[4].wait()
    for b in range(ROWS):
        for h in range(HPD):
            col = qt[h * DK : (h + 1) * DK, b : b + 1]
            ret[b : b + 1, h * DV : (h + 1) * DV] = jnp.sum(st[b, h] * col, axis=0, keepdims=True)
    wait_all("kv", KV, kv, lambda peer: sv.at[peer], rv, ssv, rsv, "recv")
    value = scale * total(rv, KV)
    wait_all("kv", KV, kv, lambda peer: sg.at[peer], rg, ssg, rsg, "recv")
    gate = scale * total(rg, KV)
    gate = gate * jax.nn.sigmoid(gate)
    rates = []
    for h in range(HPD):
        head = (tp * HPD + h).astype(F32)
        vec = jnp.full((1, 128), head, F32)
        rates.append((1.0 - jnp.exp2(-1.0 - 6.0 * vec / (HEADS - 1)))[:, 0:1])
        qk = jnp.sum(query[:, h * DK : (h + 1) * DK] * key[:, h * DK : (h + 1) * DK], axis=1, keepdims=True)
        cols = slice(h * DV, (h + 1) * DV)
        out = rates[h] * ret[:, cols] + qk * value[:, cols]
        out = out * lax.rsqrt(jnp.mean(out * out, axis=1, keepdims=True) + EPS)
        r4[pl.ds(kv, 1), :, cols] = (gate[:, cols] * out).astype(BF16)[None]

    own = lambda peer: r4.at[kv]
    start_all("kv", KV, kv, own, r4, ss4, rs4)
    ret[...] = value
    for b in range(ROWS):
        for h in range(HPD):
            col = kt[h * DK : (h + 1) * DK, b : b + 1]
            st[b, h] = rates[h] * st[b, h] + col * ret[b : b + 1, h * DV : (h + 1) * DV]
    state_copy = pltpu.make_async_copy(st, state_out_ref, lsem.at[8])
    state_copy.start()
    local[5].wait()
    wait_all("kv", KV, kv, own, r4, ss4, rs4, "recv")
    mixed = r4[...].astype(F32).reshape(128, HPD * DV).astype(BF16)
    terms = jnp.dot(mixed, wo[...], preferred_element_type=F32)
    s5[...] = terms.astype(BF16).reshape(TP, 16, 256)

    start_all("tp", TP, tp, lambda peer: s5.at[peer], r5, ss5, rs5)
    r5[tp] = s5[tp]
    wait_all("tp", TP, tp, lambda peer: s5.at[peer], r5, ss5, rs5, "recv")
    attention = total(r5, TP)
    r6[tp] = (xrows[pl.ds(pl.multiple_of(tp * 16, 16), 16), :] + attention).astype(BF16)
    mine = lambda peer: r6.at[tp]
    start_all("tp", TP, tp, mine, r6, ss6, rs6)
    wait_all("tp", TP, tp, mine, r6, ss6, rs6, "recv")
    middle = r6[...].astype(F32).reshape(128, 256)
    msquares = jnp.sum(middle * middle, axis=1, keepdims=True)
    cnormed = (middle * gains[1:2, :]).astype(BF16)

    local[6].wait()
    sb0[:, :, 0:1024] = jnp.dot(cnormed, wu[:, 0:1024], preferred_element_type=F32).astype(BF16).reshape(KV, ROWS, 1024)
    sb0[:, :, 1024:1152] = jnp.broadcast_to(msquares, (128, 128)).astype(BF16).reshape(KV, ROWS, 128)
    start_all("kv", KV, kv, lambda peer: sb0.at[peer], rb0, ssb0, rsb0)
    sb1[...] = jnp.dot(cnormed, wu[:, 1024:2048], preferred_element_type=F32).astype(BF16).reshape(KV, ROWS, 1024)
    start_all("kv", KV, kv, lambda peer: sb1.at[peer], rb1, ssb1, rsb1)
    rb0[kv] = sb0[kv]
    rb1[kv] = sb1[kv]
    midt[...] = jnp.transpose(middle)
    local[7].wait()
    wait_all("kv", KV, kv, lambda peer: sb0.at[peer], rb0, ssb0, rsb0, "recv")
    up0 = total(rb0, KV)
    cscale = lax.rsqrt(up0[:, 1024:1025] / D + EPS)
    hid0 = jnp.square(jnp.maximum(cscale * up0[:, 0:1024], 0.0)).astype(BF16)
    r7[pl.ds(kv, 1), :, 0:1024] = hid0[None]
    wait_all("kv", KV, kv, lambda peer: sb1.at[peer], rb1, ssb1, rsb1, "recv")
    hid1 = jnp.square(jnp.maximum(cscale * total(rb1, KV), 0.0)).astype(BF16)
    r7[pl.ds(kv, 1), :, 1024:2048] = hid1[None]

    own7 = lambda peer: r7.at[kv]
    start_all("kv", KV, kv, own7, r7, ss7, rs7)
    wait_all("kv", KV, kv, own7, r7, ss7, rs7, "recv")
    hidden = r7[...].astype(F32).reshape(128, 2048).astype(BF16)
    down = jnp.dot(hidden, wd[...], preferred_element_type=F32)
    s8[...] = jnp.transpose(down).astype(BF16).reshape(TP, 32, 128)

    start_all("tp", TP, tp, lambda peer: s8.at[peer], r8, ss8, rs8)
    r8[tp] = s8[tp]
    wait_all("tp", TP, tp, lambda peer: s8.at[peer], r8, ss8, rs8, "recv")
    lowered = total(r8, TP)
    out_ref[...] = (midt[pl.ds(pl.multiple_of(tp * 32, 32), 32), :] + lowered).astype(BF16)

    wait_all("tp", TP, tp, one, r1, ss1, rs1, "send")
    for s, r, a, b in ((sa, ra, ssa, rsa), (sv, rv, ssv, rsv), (sg, rg, ssg, rsg)):
        wait_all("kv", KV, kv, lambda peer: s.at[peer], r, a, b, "send")
    wait_all("kv", KV, kv, own, r4, ss4, rs4, "send")
    wait_all("tp", TP, tp, lambda peer: s5.at[peer], r5, ss5, rs5, "send")
    wait_all("tp", TP, tp, mine, r6, ss6, rs6, "send")
    wait_all("kv", KV, kv, lambda peer: sb0.at[peer], rb0, ssb0, rsb0, "send")
    wait_all("kv", KV, kv, lambda peer: sb1.at[peer], rb1, ssb1, rsb1, "send")
    wait_all("kv", KV, kv, own7, r7, ss7, rs7, "send")
    wait_all("tp", TP, tp, lambda peer: s8.at[peer], r8, ss8, rs8, "send")
    state_copy.wait()


def per_device(x, mixer_gain, channel_gain, wq, wk, wv, wg, wo, wu, wd, state):
    gains = jnp.pad(jnp.tile(jnp.stack([mixer_gain, channel_gain]), (1, 4)), ((0, 14), (0, 0)))
    vm = pl.BlockSpec(memory_space=pltpu.VMEM)
    hb = pl.BlockSpec(memory_space=pl.ANY)
    dma = pltpu.SemaphoreType.DMA
    v = lambda shape, dtype=BF16: pltpu.VMEM(shape, dtype)
    kvbuf = lambda n: v((KV, ROWS, n))
    scratch = [
        v((256, 512)), v((256, 512)), v((256, 1024)), v((256, 1024)),
        v((1024, 256)), v((256, 2048)), v((2048, 256)), v((ROWS, HPD, DK, DV), F32),
        v((48, 128)), v((TP, 48, 128)),
        kvbuf(1152), kvbuf(1152), kvbuf(1024), kvbuf(1024), kvbuf(1024), kvbuf(1024),
        kvbuf(1024), v((TP, 16, 256)), v((TP, 16, 256)), v((TP, 16, 256)),
        kvbuf(1152), kvbuf(1152), kvbuf(1024), kvbuf(1024),
        v((8, 128)), kvbuf(2048), v((TP, 32, 128)), v((TP, 32, 128)),
        v((128, 256), F32), v((512, ROWS), F32), v((512, ROWS), F32), v((ROWS, 1024), F32), v((256, 128), F32),
        dma((9,)),
        dma((TP,)), dma((TP,)),
        dma((KV,)), dma((KV,)), dma((KV,)), dma((KV,)), dma((KV,)), dma((KV,)),
        dma((KV,)), dma((KV,)), dma((TP,)), dma((TP,)), dma((TP,)), dma((TP,)),
        dma((KV,)), dma((KV,)), dma((KV,)), dma((KV,)), dma((KV,)), dma((KV,)),
        dma((TP,)), dma((TP,)),
    ]
    out, new_state = pl.pallas_call(
        kernel,
        name="layer",
        out_shape=(
            jax.ShapeDtypeStruct((32, 128), BF16),
            jax.ShapeDtypeStruct(state.shape, F32),
        ),
        in_specs=[vm, vm] + [hb] * 8,
        out_specs=(vm, hb),
        scratch_shapes=scratch,
        compiler_params=pltpu.CompilerParams(
            collective_id=0, has_side_effects=True, vmem_limit_bytes=40 * 2**20
        ),
    )(x, gains, wq, wk, wv, wg, wo, wu, wd, state)
    return out.T, new_state


def solution(mesh):
    return jax.shard_map(
        per_device,
        mesh=mesh,
        in_specs=(
            P(None, ("kv", "tp")),
            P(("kv", "tp")),
            P(("kv", "tp")),
            P("kv", "tp"),
            P("kv", "tp"),
            P("kv", "tp"),
            P("kv", "tp"),
            P("tp", "kv"),
            P("kv", "tp"),
            P("tp", "kv"),
            P("kv", "tp", None, None),
        ),
        out_specs=(P(None, ("kv", "tp")), P("kv", "tp", None, None)),
        check_vma=False,
    )
```

```python
import jax
import jax.numpy as jnp
from jax import lax
from jax.experimental import pallas as pl
from jax.experimental.pallas import tpu as pltpu
from jax.sharding import PartitionSpec as P

D = 4096
HEADS = 16
DK = 256
DV = 512
EPS = 1e-06
KV = 16
TP = 8
ROWS = 8
HPD = 2
NU = 4
UW = 2048 // NU
F32 = jnp.float32
BF16 = jnp.bfloat16
MESH = pl.DeviceIdType.MESH
HOPS = (0, 1, 2, 1)
PLANE = sorted(
    [(dz, dy) for dz in range(4) for dy in range(4) if dz or dy],
    key=lambda o: -(HOPS[o[0]] + HOPS[o[1]]),
)


def total(ref, n):
    acc = ref[0].astype(F32)
    for j in range(1, n):
        acc = acc + ref[j].astype(F32)
    return acc


def kernel(
    x_ref, mg_ref, cg_ref, wq_ref, wk_ref, wv_ref, wg_ref, wo_ref, wu_ref, wd_ref, state_ref,
    out_ref, st_ref,
    wq, wk, wv, wg, wo, wu, wd, gs,
    s1, r1, s1b, r1b, sq, rq, sk, rk, sv, rv, sg, rg, r4, s5, rd, r5, r6,
    su, ru, r7, s8, r8,
    xrows, qt, kt, ret, midt,
    lsem, ts, tr, ks, kr, plane,
):
    kv = lax.axis_index("kv")
    tp = lax.axis_index("tp")
    z, y = kv // 4, lax.rem(kv, 4)
    core, chip = lax.rem(tp, 2), tp // 2

    def plane_at(dz, dy):
        return lax.rem(z + dz, 4) * 4 + lax.rem(y + dy, 4)

    to = {o: plane_at(*o) for o in PLANE}
    come = {o: plane_at((4 - o[0]) % 4, (4 - o[1]) % 4) for o in PLANE}
    tpto = [lax.rem(tp + d, TP) for d in range(TP)]
    pair = tp + 1 - 2 * core
    sent = []

    def remote(src, dst, send, recv, device):
        return pltpu.make_async_remote_copy(
            src_ref=src, dst_ref=dst, send_sem=send, recv_sem=recv,
            device_id=device, device_id_type=MESH,
        )

    def go(copy):
        copy.start()
        sent.append(copy)

    def kv_scatter(c, s, r):
        for dz, dy in PLANE:
            o = dz * 4 + dy
            peer = to[dz, dy]
            go(remote(s.at[peer], r.at[o], ks.at[c, o], kr.at[c, o], {"kv": peer}))
        r[0] = s[kv]

    def kv_scattered(c, s, r):
        for dz, dy in PLANE:
            o = dz * 4 + dy
            remote(s.at[to[dz, dy]], r.at[o], ks.at[c, o], kr.at[c, o], {"kv": to[dz, dy]}).wait_recv()

    def kv_gather(c, r):
        for dz, dy in PLANE:
            o = dz * 4 + dy
            go(remote(r.at[kv], r.at[kv], ks.at[c, o], kr.at[c, o], {"kv": to[dz, dy]}))

    def kv_gathered(c, r):
        for dz, dy in PLANE:
            o = dz * 4 + dy
            slot = r.at[come[dz, dy]]
            remote(slot, slot, ks.at[c, o], kr.at[c, o], {"kv": to[dz, dy]}).wait_recv()

    barrier = pltpu.get_barrier_semaphore()
    ring = [{"kv": to[o]} for o in PLANE if 0 in o]
    for device in ring + [{"tp": p} for p in tpto[1:]]:
        pl.semaphore_signal(barrier, inc=1, device_id=device, device_id_type=MESH)
    first = [
        pltpu.make_async_copy(x_ref, s1b.at[0:32], lsem.at[8]),
        pltpu.make_async_copy(mg_ref, gs.at[0], lsem.at[9]),
        pltpu.make_async_copy(cg_ref, gs.at[1], lsem.at[10]),
    ]
    local = [
        pltpu.make_async_copy(a, b, lsem.at[i])
        for i, (a, b) in enumerate(
            ((wq_ref, wq), (wk_ref, wk), (wv_ref, wv), (wg_ref, wg), (state_ref, st_ref),
             (wo_ref, wo), (wu_ref, wu), (wd_ref, wd))
        )
    ]
    for c in first + local:
        c.start()
    for c in first:
        c.wait()

    r32 = lax.broadcasted_iota(jnp.int32, (32, 32), 0)
    c32 = lax.broadcasted_iota(jnp.int32, (32, 32), 1)
    column = jnp.sum(jnp.where(r32 == c32, gs[0].astype(F32), 0.0), axis=1, keepdims=True)
    s1[...] = (s1b[0:32, :].astype(F32) * column).astype(BF16)
    r1[tp] = s1[...]
    place = lax.broadcasted_iota(jnp.int32, (32, 128), 0) + 32 * lax.rem(tp, 4)
    place = jnp.where(place == lax.broadcasted_iota(jnp.int32, (32, 128), 1), 1.0, 0.0).astype(BF16)
    row = lax.broadcasted_iota(jnp.int32, (16, 32), 0)
    both = jnp.where(row == 0, gs[1].astype(F32), 0.0).astype(BF16)
    s1b[32:48, :] = jnp.dot(both, place, preferred_element_type=F32).astype(BF16)
    r1b[tp] = s1b[...]
    pl.semaphore_wait(barrier, len(ring) + TP - 1)

    for d in (5, 4, 3, 6, 2, 7, 1):
        go(remote(s1, r1.at[tp], ts.at[0, d], tr.at[0, d], {"tp": tpto[d]}))
    for d in (5, 4, 3, 6, 2, 7, 1):
        go(remote(s1b, r1b.at[tp], ts.at[1, d], tr.at[1, d], {"tp": tpto[d]}))
    for o in PLANE:
        if o[1] == 0:
            pl.semaphore_signal(plane, inc=1, device_id={"kv": to[o]}, device_id_type=MESH)
    for d in range(1, TP):
        remote(s1, r1.at[tpto[TP - d]], ts.at[0, d], tr.at[0, d], {"tp": tpto[d]}).wait_recv()
    normed = jnp.transpose(r1[...].astype(F32).reshape(256, 128)).astype(BF16)

    local[0].wait()
    sq[...] = jnp.dot(normed, wq[...], preferred_element_type=F32).astype(BF16).reshape(KV, ROWS, 512)
    pl.semaphore_wait(plane, 3)
    kv_scatter(0, sq, rq)
    local[1].wait()
    sk[...] = jnp.dot(normed, wk[...], preferred_element_type=F32).astype(BF16).reshape(KV, ROWS, 512)
    kv_scatter(1, sk, rk)
    for d in range(1, TP):
        remote(s1b, r1b.at[tpto[TP - d]], ts.at[1, d], tr.at[1, d], {"tp": tpto[d]}).wait_recv()
    x = jnp.transpose(jnp.concatenate([r1b[j, 0:32, :].astype(F32) for j in range(TP)], axis=0))
    xrows[...] = x.reshape(2, 64, 256)
    squares = jnp.sum(x * x, axis=1, keepdims=True)
    local[2].wait()
    sv[:, :, 0:1024] = jnp.dot(normed, wv[...], preferred_element_type=F32).astype(BF16).reshape(KV, ROWS, 1024)
    sv[:, :, 1024:1152] = jnp.broadcast_to(squares, (128, 128)).astype(BF16).reshape(KV, ROWS, 128)
    kv_scatter(2, sv, rv)
    local[3].wait()
    for h in range(HPD):
        part = jnp.dot(normed, wg[:, h * DV : (h + 1) * DV], preferred_element_type=F32)
        sg[h] = part.astype(BF16).reshape(KV, ROWS, DV)
        kv_scatter(3 + h, sg.at[h], rg.at[h])

    kv_scattered(0, sq, rq)
    query = total(rq, KV)
    qt[...] = jnp.transpose(query)
    kv_scattered(1, sk, rk)
    key = total(rk, KV)
    local[4].wait()
    for b in range(ROWS):
        for h in range(HPD):
            col = qt[h * DK : (h + 1) * DK, b : b + 1]
            ret[b : b + 1, h * DV : (h + 1) * DV] = jnp.sum(st_ref[b, h] * col, axis=0, keepdims=True)
    kv_scattered(2, sv, rv)
    sums = total(rv, KV)
    scale = lax.rsqrt(sums[:, 1024:1025] / D + EPS)
    value = scale * sums[:, 0:1024]
    query = scale * query
    key = scale * key * DK ** (-0.5)
    kt[...] = jnp.transpose(key)
    rates, outs = [], []
    for h in range(HPD):
        head = jnp.full((1, 128), (tp * HPD + h).astype(F32), F32)
        rates.append((1.0 - jnp.exp2(-1.0 - 6.0 * head / (HEADS - 1)))[:, 0:1])
        keys = slice(h * DK, (h + 1) * DK)
        cols = slice(h * DV, (h + 1) * DV)
        qk = jnp.sum(query[:, keys] * key[:, keys], axis=1, keepdims=True)
        out = rates[h] * (scale * ret[:, cols]) + qk * value[:, cols]
        outs.append(out * lax.rsqrt(jnp.mean(out * out, axis=1, keepdims=True) + EPS))
    for h in range(HPD):
        kv_scattered(3 + h, sg.at[h], rg.at[h])
        gate = scale * total(rg.at[h], KV)
        r4[h, kv] = (gate * jax.nn.sigmoid(gate) * outs[h]).astype(BF16)
        kv_gather(5 + h, r4.at[h])

    ret[...] = value
    for b in range(ROWS):
        for h in range(HPD):
            col = kt[h * DK : (h + 1) * DK, b : b + 1]
            st_ref[b, h] = rates[h] * st_ref[b, h] + col * ret[b : b + 1, h * DV : (h + 1) * DV]

    local[5].wait()
    terms = jnp.zeros((128, 256), F32)
    for h in range(HPD):
        kv_gathered(5 + h, r4.at[h])
        mixed = r4[h].astype(F32).reshape(128, DV).astype(BF16)
        terms = terms + jnp.dot(mixed, wo[h * DV : (h + 1) * DV, :], preferred_element_type=F32)
    s5[...] = terms.astype(BF16).reshape(2, 64, 256)
    swap = remote(s5.at[1 - core], rd, ts.at[2, 0], tr.at[2, 0], {"tp": pair})
    go(swap)
    swap.wait_recv()
    r5[chip] = (s5[core].astype(F32) + rd[...].astype(F32)).astype(BF16)
    for d in (4, 2, 6):
        go(remote(r5.at[chip], r5.at[chip], ts.at[2, d], tr.at[2, d], {"tp": tpto[d]}))
    for d in (2, 6, 4):
        slot = r5.at[tpto[TP - d] // 2]
        remote(slot, slot, ts.at[2, d], tr.at[2, d], {"tp": tpto[d]}).wait_recv()
    r6[core] = (xrows[core] + total(r5, 4)).astype(BF16)
    go(remote(r6.at[core], r6.at[core], ts.at[2, 1], tr.at[2, 1], {"tp": pair}))
    local[6].wait()
    remote(r6.at[1 - core], r6.at[1 - core], ts.at[2, 1], tr.at[2, 1], {"tp": pair}).wait_recv()
    middle = r6[...].astype(F32).reshape(128, 256)
    gains = jnp.concatenate(
        [sum(r1b[j, 32:48, :].astype(F32) for j in range(4 * i, 4 * i + 4)) for i in range(2)], axis=1
    )
    cnormed = (middle * gains[0:1, :]).astype(BF16)

    for c in range(NU):
        if c == 0:
            msquares = jnp.sum(middle * middle, axis=1, keepdims=True)
            su[0, :, :, UW : UW + 128] = jnp.broadcast_to(msquares, (128, 128)).astype(BF16).reshape(KV, ROWS, 128)
        part = jnp.dot(cnormed, wu[:, c * UW : (c + 1) * UW], preferred_element_type=F32)
        su[c, :, :, 0:UW] = part.astype(BF16).reshape(KV, ROWS, UW)
        if c == 0:
            kv_scatter(7, su.at[0], ru.at[0])
        else:
            kv_scatter(7 + c, su.at[c, :, :, 0:UW], ru.at[c, :, :, 0:UW])
    midt[...] = jnp.transpose(middle)
    for c in range(NU):
        if c == 0:
            kv_scattered(7, su.at[0], ru.at[0])
        else:
            kv_scattered(7 + c, su.at[c, :, :, 0:UW], ru.at[c, :, :, 0:UW])
        if c == 0:
            up = total(ru.at[0], KV)
            cscale = lax.rsqrt(up[:, UW : UW + 1] / D + EPS)
            up = up[:, 0:UW]
        else:
            up = total(ru.at[c, :, :, 0:UW], KV)
        r7[c, kv] = jnp.square(jnp.maximum(cscale * up, 0.0)).astype(BF16)
        kv_gather(7 + NU + c, r7.at[c])

    local[7].wait()
    down = jnp.zeros((128, 256), F32)
    for c in range(NU):
        kv_gathered(7 + NU + c, r7.at[c])
        hidden = r7[c].astype(F32).reshape(128, UW).astype(BF16)
        down = down + jnp.dot(hidden, wd[c * UW : (c + 1) * UW, :], preferred_element_type=F32)
    s8[...] = jnp.transpose(down).astype(BF16).reshape(TP, 32, 128)
    for d in (5, 4, 3, 6, 2, 7, 1):
        go(remote(s8.at[tpto[d]], r8.at[d], ts.at[3, d], tr.at[3, d], {"tp": tpto[d]}))
    r8[0] = s8[tp]
    for d in range(1, TP):
        remote(s8.at[tpto[d]], r8.at[d], ts.at[3, d], tr.at[3, d], {"tp": tpto[d]}).wait_recv()
    lowered = total(r8, TP)
    out_ref[...] = (midt[pl.ds(pl.multiple_of(tp * 32, 32), 32), :] + lowered).astype(BF16)
    for copy in sent:
        copy.wait_send()


def writer(a_ref, s_ref, out_ref, state_ref, sem):
    copies = [pltpu.make_async_copy(a_ref, out_ref, sem.at[ROWS])]
    copies += [pltpu.make_async_copy(s_ref.at[b], state_ref.at[b], sem.at[b]) for b in range(ROWS)]
    for c in copies:
        c.start()
    for c in copies:
        c.wait()


def per_device(x, mixer_gain, channel_gain, wq, wk, wv, wg, wo, wu, wd, state):
    vm = pl.BlockSpec(memory_space=pltpu.VMEM)
    hb = pl.BlockSpec(memory_space=pltpu.HBM)
    dma = pltpu.SemaphoreType.DMA
    v = lambda *shape: pltpu.VMEM(shape, BF16)
    f = lambda *shape: pltpu.VMEM(shape, F32)
    scratch = [
        v(256, 512), v(256, 512), v(256, 1024), v(256, 1024), v(1024, 256), v(256, 2048), v(2048, 256), v(2, 1, 32),
        v(32, 128), v(TP, 32, 128), v(48, 128), v(TP, 48, 128),
        v(KV, ROWS, 512), v(KV, ROWS, 512), v(KV, ROWS, 512), v(KV, ROWS, 512),
        v(KV, ROWS, 1152), v(KV, ROWS, 1152), v(HPD, KV, ROWS, DV), v(HPD, KV, ROWS, DV),
        v(HPD, KV, ROWS, DV), v(2, 64, 256), v(64, 256), v(4, 64, 256), v(2, 64, 256),
        v(NU, KV, ROWS, UW + 128), v(NU, KV, ROWS, UW + 128), v(NU, KV, ROWS, UW),
        v(TP, 32, 128), v(TP, 32, 128),
        f(2, 64, 256), f(512, ROWS), f(512, ROWS), f(ROWS, 1024), f(256, 128),
        dma((11,)), dma((4, TP)), dma((4, TP)), dma((7 + 2 * NU, KV)), dma((7 + 2 * NU, KV)),
        pltpu.SemaphoreType.REGULAR,
    ]
    out, new_state = pl.pallas_call(
        kernel,
        name="layer",
        out_shape=(pltpu.VMEM((32, 128), BF16), pltpu.VMEM(state.shape, F32)),
        in_specs=[hb] * 11,
        out_specs=(vm, vm),
        scratch_shapes=scratch,
        compiler_params=pltpu.CompilerParams(
            collective_id=0, has_side_effects=True, vmem_limit_bytes=int(55.7 * 2**20)
        ),
    )(x.T, mixer_gain.reshape(1, 32), channel_gain.reshape(1, 32), wq, wk, wv, wg, wo, wu, wd, state)
    out, new_state = pl.pallas_call(
        writer,
        name="writer",
        out_shape=(jax.ShapeDtypeStruct((32, 128), BF16), jax.ShapeDtypeStruct(state.shape, F32)),
        in_specs=[vm, vm],
        out_specs=(hb, hb),
        scratch_shapes=[dma((ROWS + 1,))],
        compiler_params=pltpu.CompilerParams(vmem_limit_bytes=2**20),
    )(out, new_state)
    return out.T, new_state


def solution(mesh):
    return jax.shard_map(
        per_device,
        mesh=mesh,
        in_specs=(
            P(None, ("kv", "tp")),
            P(("kv", "tp")),
            P(("kv", "tp")),
            P("kv", "tp"),
            P("kv", "tp"),
            P("kv", "tp"),
            P("kv", "tp"),
            P("tp", "kv"),
            P("kv", "tp"),
            P("tp", "kv"),
            P("kv", "tp", None, None),
        ),
        out_specs=(P(None, ("kv", "tp")), P("kv", "tp", None, None)),
        check_vma=False,
    )
```

```python
import jax
import jax.numpy as jnp
from jax import lax
from jax.experimental import pallas as pl
from jax.experimental.pallas import tpu as pltpu
from jax.sharding import PartitionSpec as P

D = 4096
HEADS = 16
DK = 256
DV = 512
EPS = 1e-06
KV = 16
TP = 8
ROWS = 8
HPD = 2
NU = 4
UW = 2048 // NU
F32 = jnp.float32
BF16 = jnp.bfloat16
MESH = pl.DeviceIdType.MESH
HOPS = (0, 1, 2, 1)
PLANE = sorted(
    [(dz, dy) for dz in range(4) for dy in range(4) if dz or dy],
    key=lambda o: -(HOPS[o[0]] + HOPS[o[1]]),
)


def total(ref, n):
    acc = ref[0].astype(F32)
    for j in range(1, n):
        acc = acc + ref[j].astype(F32)
    return acc


def kernel(
    x_ref, mg_ref, cg_ref, wq_ref, wk_ref, wv_ref, wg_ref, wo_ref, wu_ref, wd_ref, state_ref,
    out_ref, st_ref,
    wq, wk, wv, wg, wo, wu, wd, gs,
    s1, r1, s1b, r1b, sq, rq, sk, rk, sv, rv, sg, rg, r4, s5, rd, r5, r6,
    su, ru, r7, s8, r8,
    xrows, qt, kt, ret, midt,
    lsem, ts, tr, ks, kr, plane,
):
    kv = lax.axis_index("kv")
    tp = lax.axis_index("tp")
    z, y = kv // 4, lax.rem(kv, 4)
    core, chip = lax.rem(tp, 2), tp // 2

    def plane_at(dz, dy):
        return lax.rem(z + dz, 4) * 4 + lax.rem(y + dy, 4)

    to = {o: plane_at(*o) for o in PLANE}
    tpto = [lax.rem(tp + d, TP) for d in range(TP)]
    pair = tp + 1 - 2 * core
    sent = []

    def remote(src, dst, send, recv, device):
        return pltpu.make_async_remote_copy(
            src_ref=src, dst_ref=dst, send_sem=send, recv_sem=recv,
            device_id=device, device_id_type=MESH,
        )

    def step(sems, i, slots, device):
        whole = remote(slots, slots, sems[0].at[i], sems[1].at[i], device)
        sent.append(whole)
        return whole

    ksem, tsem = (ks, kr), (ts, tr)
    aside, across = {"kv": to[0, 1]}, {"tp": tpto[1]}

    def kv_scatter(c, s, r):
        for dz, dy in PLANE:
            peer = to[dz, dy]
            remote(s.at[peer], r.at[dz * 4 + dy], ks.at[c], kr.at[c], {"kv": peer}).start()
        r[0] = s[kv]
        return step(ksem, c, r.at[1:KV], aside)

    def kv_gather(c, r):
        for o in PLANE:
            remote(r.at[kv], r.at[kv], ks.at[c], kr.at[c], {"kv": to[o]}).start()
        return step(ksem, c, r.at[1:KV], aside)

    barrier = pltpu.get_barrier_semaphore()
    ring = [{"kv": to[o]} for o in PLANE if 0 in o]
    for device in ring + [{"tp": p} for p in tpto[1:]]:
        pl.semaphore_signal(barrier, inc=1, device_id=device, device_id_type=MESH)
    first = [
        pltpu.make_async_copy(x_ref, s1b.at[0:32], lsem.at[8]),
        pltpu.make_async_copy(mg_ref, gs.at[0], lsem.at[9]),
        pltpu.make_async_copy(cg_ref, gs.at[1], lsem.at[10]),
    ]
    local = [
        pltpu.make_async_copy(a, b, lsem.at[i])
        for i, (a, b) in enumerate(
            ((wq_ref, wq), (wk_ref, wk), (wv_ref, wv), (wg_ref, wg), (state_ref, st_ref),
             (wo_ref, wo), (wu_ref, wu), (wd_ref, wd))
        )
    ]
    for c in first + local:
        c.start()
    for c in first:
        c.wait()

    r32 = lax.broadcasted_iota(jnp.int32, (32, 32), 0)
    c32 = lax.broadcasted_iota(jnp.int32, (32, 32), 1)
    column = jnp.sum(jnp.where(r32 == c32, gs[0].astype(F32), 0.0), axis=1, keepdims=True)
    s1[...] = (s1b[0:32, :].astype(F32) * column).astype(BF16)
    r1[tp] = s1[...]
    place = lax.broadcasted_iota(jnp.int32, (32, 128), 0) + 32 * lax.rem(tp, 4)
    place = jnp.where(place == lax.broadcasted_iota(jnp.int32, (32, 128), 1), 1.0, 0.0).astype(BF16)
    row = lax.broadcasted_iota(jnp.int32, (16, 32), 0)
    both = jnp.where(row == 0, gs[1].astype(F32), 0.0).astype(BF16)
    s1b[32:48, :] = jnp.dot(both, place, preferred_element_type=F32).astype(BF16)
    r1b[tp] = s1b[...]
    pl.semaphore_wait(barrier, len(ring) + TP - 1)

    for d in (5, 4, 3, 6, 2, 7, 1):
        remote(s1, r1.at[tp], ts.at[0], tr.at[0], {"tp": tpto[d]}).start()
    for d in (5, 4, 3, 6, 2, 7, 1):
        remote(s1b, r1b.at[tp], ts.at[1], tr.at[1], {"tp": tpto[d]}).start()
    first_in = step(tsem, 0, r1.at[1:TP], across)
    second_in = step(tsem, 1, r1b.at[1:TP], across)
    for o in PLANE:
        if o[1] == 0:
            pl.semaphore_signal(plane, inc=1, device_id={"kv": to[o]}, device_id_type=MESH)
    first_in.wait_recv()
    normed = jnp.transpose(r1[...].astype(F32).reshape(256, 128)).astype(BF16)

    local[0].wait()
    sq[...] = jnp.dot(normed, wq[...], preferred_element_type=F32).astype(BF16).reshape(KV, ROWS, 512)
    pl.semaphore_wait(plane, 3)
    query_in = kv_scatter(0, sq, rq)
    local[1].wait()
    sk[...] = jnp.dot(normed, wk[...], preferred_element_type=F32).astype(BF16).reshape(KV, ROWS, 512)
    key_in = kv_scatter(1, sk, rk)
    second_in.wait_recv()
    x = jnp.transpose(jnp.concatenate([r1b[j, 0:32, :].astype(F32) for j in range(TP)], axis=0))
    xrows[...] = x.reshape(2, 64, 256)
    squares = jnp.sum(x * x, axis=1, keepdims=True)
    local[2].wait()
    sv[:, :, 0:1024] = jnp.dot(normed, wv[...], preferred_element_type=F32).astype(BF16).reshape(KV, ROWS, 1024)
    sv[:, :, 1024:1152] = jnp.broadcast_to(squares, (128, 128)).astype(BF16).reshape(KV, ROWS, 128)
    value_in = kv_scatter(2, sv, rv)
    local[3].wait()
    gate_in, mixed_in = [], []
    for h in range(HPD):
        part = jnp.dot(normed, wg[:, h * DV : (h + 1) * DV], preferred_element_type=F32)
        sg[h] = part.astype(BF16).reshape(KV, ROWS, DV)
        gate_in.append(kv_scatter(3 + h, sg.at[h], rg.at[h]))

    query_in.wait_recv()
    query = total(rq, KV)
    qt[...] = jnp.transpose(query)
    key_in.wait_recv()
    key = total(rk, KV)
    local[4].wait()
    for b in range(ROWS):
        for h in range(HPD):
            col = qt[h * DK : (h + 1) * DK, b : b + 1]
            ret[b : b + 1, h * DV : (h + 1) * DV] = jnp.sum(st_ref[b, h] * col, axis=0, keepdims=True)
    value_in.wait_recv()
    sums = total(rv, KV)
    scale = lax.rsqrt(sums[:, 1024:1025] / D + EPS)
    value = scale * sums[:, 0:1024]
    query = scale * query
    key = scale * key * DK ** (-0.5)
    kt[...] = jnp.transpose(key)
    rates, outs = [], []
    for h in range(HPD):
        head = jnp.full((1, 128), (tp * HPD + h).astype(F32), F32)
        rates.append((1.0 - jnp.exp2(-1.0 - 6.0 * head / (HEADS - 1)))[:, 0:1])
        keys = slice(h * DK, (h + 1) * DK)
        cols = slice(h * DV, (h + 1) * DV)
        qk = jnp.sum(query[:, keys] * key[:, keys], axis=1, keepdims=True)
        out = rates[h] * (scale * ret[:, cols]) + qk * value[:, cols]
        outs.append(out * lax.rsqrt(jnp.mean(out * out, axis=1, keepdims=True) + EPS))
    for h in range(HPD):
        gate_in[h].wait_recv()
        gate = scale * total(rg.at[h], KV)
        r4[h, kv] = (gate * jax.nn.sigmoid(gate) * outs[h]).astype(BF16)
        mixed_in.append(kv_gather(5 + h, r4.at[h]))

    ret[...] = value
    for b in range(ROWS):
        for h in range(HPD):
            col = kt[h * DK : (h + 1) * DK, b : b + 1]
            st_ref[b, h] = rates[h] * st_ref[b, h] + col * ret[b : b + 1, h * DV : (h + 1) * DV]

    local[5].wait()
    terms = jnp.zeros((128, 256), F32)
    for h in range(HPD):
        mixed_in[h].wait_recv()
        mixed = r4[h].astype(F32).reshape(128, DV).astype(BF16)
        terms = terms + jnp.dot(mixed, wo[h * DV : (h + 1) * DV, :], preferred_element_type=F32)
    s5[...] = terms.astype(BF16).reshape(2, 64, 256)
    mate = {"tp": pair}
    remote(s5.at[1 - core], rd, ts.at[2], tr.at[2], mate).start()
    step(tsem, 2, rd, mate).wait_recv()
    r5[chip] = (s5[core].astype(F32) + rd[...].astype(F32)).astype(BF16)
    for d in (4, 2, 6):
        remote(r5.at[chip], r5.at[chip], ts.at[3], tr.at[3], {"tp": tpto[d]}).start()
    step(tsem, 3, r5.at[1:4], across).wait_recv()
    r6[core] = (xrows[core] + total(r5, 4)).astype(BF16)
    remote(r6.at[core], r6.at[core], ts.at[4], tr.at[4], mate).start()
    local[6].wait()
    step(tsem, 4, r6.at[1 - core], mate).wait_recv()
    middle = r6[...].astype(F32).reshape(128, 256)
    gains = jnp.concatenate(
        [sum(r1b[j, 32:48, :].astype(F32) for j in range(4 * i, 4 * i + 4)) for i in range(2)], axis=1
    )
    cnormed = (middle * gains[0:1, :]).astype(BF16)

    up_in, hidden_in = [], []
    for c in range(NU):
        if c == 0:
            msquares = jnp.sum(middle * middle, axis=1, keepdims=True)
            su[0, :, :, UW : UW + 128] = jnp.broadcast_to(msquares, (128, 128)).astype(BF16).reshape(KV, ROWS, 128)
        part = jnp.dot(cnormed, wu[:, c * UW : (c + 1) * UW], preferred_element_type=F32)
        su[c, :, :, 0:UW] = part.astype(BF16).reshape(KV, ROWS, UW)
        width = UW + 128 if c == 0 else UW
        up_in.append(kv_scatter(7 + c, su.at[c, :, :, 0:width], ru.at[c, :, :, 0:width]))
    midt[...] = jnp.transpose(middle)
    for c in range(NU):
        up_in[c].wait_recv()
        if c == 0:
            up = total(ru.at[0], KV)
            cscale = lax.rsqrt(up[:, UW : UW + 1] / D + EPS)
            up = up[:, 0:UW]
        else:
            up = total(ru.at[c, :, :, 0:UW], KV)
        r7[c, kv] = jnp.square(jnp.maximum(cscale * up, 0.0)).astype(BF16)
        hidden_in.append(kv_gather(7 + NU + c, r7.at[c]))

    local[7].wait()
    down = jnp.zeros((128, 256), F32)
    for c in range(NU):
        hidden_in[c].wait_recv()
        hidden = r7[c].astype(F32).reshape(128, UW).astype(BF16)
        down = down + jnp.dot(hidden, wd[c * UW : (c + 1) * UW, :], preferred_element_type=F32)
    s8[...] = jnp.transpose(down).astype(BF16).reshape(TP, 32, 128)
    for d in (5, 4, 3, 6, 2, 7, 1):
        remote(s8.at[tpto[d]], r8.at[d], ts.at[5], tr.at[5], {"tp": tpto[d]}).start()
    r8[0] = s8[tp]
    step(tsem, 5, r8.at[1:TP], across).wait_recv()
    lowered = total(r8, TP)
    out_ref[...] = (midt[pl.ds(pl.multiple_of(tp * 32, 32), 32), :] + lowered).astype(BF16)
    for copy in sent:
        copy.wait_send()


def writer(a_ref, s_ref, out_ref, state_ref, sem):
    copies = [pltpu.make_async_copy(a_ref, out_ref, sem.at[ROWS])]
    copies += [pltpu.make_async_copy(s_ref.at[b], state_ref.at[b], sem.at[b]) for b in range(ROWS)]
    for c in copies:
        c.start()
    for c in copies:
        c.wait()


def per_device(x, mixer_gain, channel_gain, wq, wk, wv, wg, wo, wu, wd, state):
    vm = pl.BlockSpec(memory_space=pltpu.VMEM)
    hb = pl.BlockSpec(memory_space=pltpu.HBM)
    dma = pltpu.SemaphoreType.DMA
    v = lambda *shape: pltpu.VMEM(shape, BF16)
    f = lambda *shape: pltpu.VMEM(shape, F32)
    scratch = [
        v(256, 512), v(256, 512), v(256, 1024), v(256, 1024), v(1024, 256), v(256, 2048), v(2048, 256), v(2, 1, 32),
        v(32, 128), v(TP, 32, 128), v(48, 128), v(TP, 48, 128),
        v(KV, ROWS, 512), v(KV, ROWS, 512), v(KV, ROWS, 512), v(KV, ROWS, 512),
        v(KV, ROWS, 1152), v(KV, ROWS, 1152), v(HPD, KV, ROWS, DV), v(HPD, KV, ROWS, DV),
        v(HPD, KV, ROWS, DV), v(2, 64, 256), v(64, 256), v(4, 64, 256), v(2, 64, 256),
        v(NU, KV, ROWS, UW + 128), v(NU, KV, ROWS, UW + 128), v(NU, KV, ROWS, UW),
        v(TP, 32, 128), v(TP, 32, 128),
        f(2, 64, 256), f(512, ROWS), f(512, ROWS), f(ROWS, 1024), f(256, 128),
        dma((11,)), dma((6,)), dma((6,)), dma((7 + 2 * NU,)), dma((7 + 2 * NU,)),
        pltpu.SemaphoreType.REGULAR,
    ]
    out, new_state = pl.pallas_call(
        kernel,
        name="layer",
        out_shape=(pltpu.VMEM((32, 128), BF16), pltpu.VMEM(state.shape, F32)),
        in_specs=[hb] * 11,
        out_specs=(vm, vm),
        scratch_shapes=scratch,
        compiler_params=pltpu.CompilerParams(
            collective_id=0, has_side_effects=True, vmem_limit_bytes=int(55.7 * 2**20)
        ),
    )(x.T, mixer_gain.reshape(1, 32), channel_gain.reshape(1, 32), wq, wk, wv, wg, wo, wu, wd, state)
    out, new_state = pl.pallas_call(
        writer,
        name="writer",
        out_shape=(jax.ShapeDtypeStruct((32, 128), BF16), jax.ShapeDtypeStruct(state.shape, F32)),
        in_specs=[vm, vm],
        out_specs=(hb, hb),
        scratch_shapes=[dma((ROWS + 1,))],
        compiler_params=pltpu.CompilerParams(vmem_limit_bytes=2**20),
    )(out, new_state)
    return out.T, new_state


def solution(mesh):
    return jax.shard_map(
        per_device,
        mesh=mesh,
        in_specs=(
            P(None, ("kv", "tp")),
            P(("kv", "tp")),
            P(("kv", "tp")),
            P("kv", "tp"),
            P("kv", "tp"),
            P("kv", "tp"),
            P("kv", "tp"),
            P("tp", "kv"),
            P("kv", "tp"),
            P("tp", "kv"),
            P("kv", "tp", None, None),
        ),
        out_specs=(P(None, ("kv", "tp")), P("kv", "tp", None, None)),
        check_vma=False,
    )
```

```python
import jax
import jax.numpy as jnp
from jax import lax
from jax.experimental import pallas as pl
from jax.experimental.pallas import tpu as pltpu
from jax.sharding import PartitionSpec as P

D = 4096
HEADS = 16
DK = 256
DV = 512
EPS = 1e-06
KV = 16
TP = 8
ROWS = 8
HPD = 2
NU = 4
UW = 2048 // NU
F32 = jnp.float32
BF16 = jnp.bfloat16
MESH = pl.DeviceIdType.MESH
HOPS = (0, 1, 2, 1)
PLANE = sorted(
    [(dz, dy) for dz in range(4) for dy in range(4) if dz or dy],
    key=lambda o: -(HOPS[o[0]] + HOPS[o[1]]),
)


def total(ref, n):
    acc = ref[0].astype(F32)
    for j in range(1, n):
        acc = acc + ref[j].astype(F32)
    return acc


def kernel(
    x_ref, mg_ref, cg_ref, wq_ref, wk_ref, wv_ref, wg_ref, wo_ref, wu_ref, wd_ref, state_ref,
    out_ref, st_ref,
    wq, wk, wv, wg, wo, wu, wd, gs,
    s1, r1, s1b, r1b, sq, rq, tq, uq, sk, rk, tk, uk, sv, rv, tv, uv, sg, rg, tg, ug, r4, s5, rd, r5, r6,
    su, ru, r7, s8, r8,
    xrows, tacc, qt, kt, ret, midt,
    lsem, ts, tr, ks, kr, plane,
):
    kv = lax.axis_index("kv")
    tp = lax.axis_index("tp")
    z, y = kv // 4, lax.rem(kv, 4)
    core, chip = lax.rem(tp, 2), tp // 2

    def plane_at(dz, dy):
        return lax.rem(z + dz, 4) * 4 + lax.rem(y + dy, 4)

    to = {o: plane_at(*o) for o in PLANE}
    tpto = [lax.rem(tp + d, TP) for d in range(TP)]
    pair = tp + 1 - 2 * core
    sent = []

    def remote(src, dst, send, recv, device):
        return pltpu.make_async_remote_copy(
            src_ref=src, dst_ref=dst, send_sem=send, recv_sem=recv,
            device_id=device, device_id_type=MESH,
        )

    def step(sems, i, slots, device):
        whole = remote(slots, slots, sems[0].at[i], sems[1].at[i], device)
        sent.append(whole)
        return whole

    ksem, tsem = (ks, kr), (ts, tr)
    aside, across = {"kv": to[0, 1]}, {"tp": tpto[1]}

    ring_at = {"z": (z, lambda q: {"kv": q * 4 + y}), "y": (y, lambda q: {"kv": z * 4 + q})}

    def ring_scatter(c, axis, s, r):
        me, device = ring_at[axis]
        part = (lambda q: s.at[q]) if axis == "z" else (lambda q: s.at[:, q])
        for d in (2, 1, 3):
            q = lax.rem(me + d, 4)
            remote(part(q), r.at[d], ks.at[c], kr.at[c], device(q)).start()
        r[0] = part(me)[...]
        return step(ksem, c, r.at[1:4], aside)

    def ring_finish(stage, c, axis, r, t, u):
        me, device = ring_at[axis]
        stage.wait_recv()
        t[...] = total(r, 4).astype(BF16)
        for d in (2, 1, 3):
            q = lax.rem(me + d, 4)
            remote(t.at[q], u.at[d], ks.at[c], kr.at[c], device(q)).start()
        u[0] = t[me]
        return step(ksem, c, u.at[1:4], aside)

    def kv_gather(c, r):
        for o in PLANE:
            remote(r.at[kv], r.at[kv], ks.at[c], kr.at[c], {"kv": to[o]}).start()
        return step(ksem, c, r.at[1:KV], aside)

    barrier = pltpu.get_barrier_semaphore()
    ring = [{"kv": to[o]} for o in PLANE if 0 in o]
    for device in ring + [{"tp": p} for p in tpto[1:]]:
        pl.semaphore_signal(barrier, inc=1, device_id=device, device_id_type=MESH)
    first = [
        pltpu.make_async_copy(x_ref, s1b.at[0:32], lsem.at[8]),
        pltpu.make_async_copy(mg_ref, gs.at[0], lsem.at[9]),
        pltpu.make_async_copy(cg_ref, gs.at[1], lsem.at[10]),
    ]
    local = [
        pltpu.make_async_copy(a, b, lsem.at[i])
        for i, (a, b) in enumerate(
            ((wq_ref, wq), (wk_ref, wk), (wv_ref, wv), (wg_ref, wg), (state_ref, st_ref),
             (wo_ref, wo), (wu_ref, wu), (wd_ref, wd))
        )
    ]
    for c in first + local:
        c.start()
    for c in first:
        c.wait()

    r32 = lax.broadcasted_iota(jnp.int32, (32, 32), 0)
    c32 = lax.broadcasted_iota(jnp.int32, (32, 32), 1)
    column = jnp.sum(jnp.where(r32 == c32, gs[0].astype(F32), 0.0), axis=1, keepdims=True)
    s1[...] = (s1b[0:32, :].astype(F32) * column).astype(BF16)
    r1[tp] = s1[...]
    place = lax.broadcasted_iota(jnp.int32, (32, 128), 0) + 32 * lax.rem(tp, 4)
    place = jnp.where(place == lax.broadcasted_iota(jnp.int32, (32, 128), 1), 1.0, 0.0).astype(BF16)
    row = lax.broadcasted_iota(jnp.int32, (16, 32), 0)
    both = jnp.where(row == 0, gs[1].astype(F32), 0.0).astype(BF16)
    s1b[32:48, :] = jnp.dot(both, place, preferred_element_type=F32).astype(BF16)
    r1b[tp] = s1b[...]
    pl.semaphore_wait(barrier, len(ring) + TP - 1)

    for d in (5, 4, 3, 6, 2, 7, 1):
        remote(s1, r1.at[tp], ts.at[0], tr.at[0], {"tp": tpto[d]}).start()
    for d in (5, 4, 3, 6, 2, 7, 1):
        remote(s1b, r1b.at[tp], ts.at[1], tr.at[1], {"tp": tpto[d]}).start()
    first_in = step(tsem, 0, r1.at[1:TP], across)
    second_in = step(tsem, 1, r1b.at[1:TP], across)
    for o in PLANE:
        if o[1] == 0:
            pl.semaphore_signal(plane, inc=1, device_id={"kv": to[o]}, device_id_type=MESH)
    first_in.wait_recv()
    normed = jnp.transpose(r1[...].astype(F32).reshape(256, 128)).astype(BF16)

    local[0].wait()
    sq[...] = jnp.dot(normed, wq[...], preferred_element_type=F32).reshape(4, 4, ROWS, 512).astype(BF16)
    pl.semaphore_wait(plane, 3)
    query_in = ring_scatter(0, "z", sq, rq)
    local[1].wait()
    sk[...] = jnp.dot(normed, wk[...], preferred_element_type=F32).reshape(4, 4, ROWS, 512).astype(BF16)
    key_in = ring_scatter(1, "z", sk, rk)
    second_in.wait_recv()
    x = jnp.transpose(jnp.concatenate([r1b[j, 0:32, :].astype(F32) for j in range(TP)], axis=0))
    xrows[...] = x.reshape(2, 64, 256)
    squares = jnp.sum(x * x, axis=1, keepdims=True)
    local[2].wait()
    sv[:, :, :, 0:1024] = jnp.dot(normed, wv[...], preferred_element_type=F32).reshape(4, 4, ROWS, 1024).astype(BF16)
    sv[:, :, :, 1024:1152] = jnp.broadcast_to(squares, (128, 128)).reshape(4, 4, ROWS, 128).astype(BF16)
    value_in = ring_scatter(2, "y", sv, rv)
    local[3].wait()
    gate_in, mixed_in = [], []
    for h in range(HPD):
        part = jnp.dot(normed, wg[:, h * DV : (h + 1) * DV], preferred_element_type=F32)
        sg[h] = part.reshape(4, 4, ROWS, DV).astype(BF16)
        gate_in.append(ring_scatter(3 + h, "zy"[h], sg.at[h], rg.at[h]))

    query_in = ring_finish(query_in, 7 + 2 * NU, "y", rq, tq, uq)
    key_in = ring_finish(key_in, 7 + 2 * NU + 1, "y", rk, tk, uk)
    value_in = ring_finish(value_in, 7 + 2 * NU + 2, "z", rv, tv, uv)
    for h in range(HPD):
        gate_in[h] = ring_finish(gate_in[h], 10 + 2 * NU + h, "yz"[h], rg.at[h], tg.at[h], ug.at[h])
    query_in.wait_recv()
    query = total(uq, 4)
    qt[...] = jnp.transpose(query)
    key_in.wait_recv()
    key = total(uk, 4)
    local[4].wait()
    for b in range(ROWS):
        for h in range(HPD):
            col = qt[h * DK : (h + 1) * DK, b : b + 1]
            ret[b : b + 1, h * DV : (h + 1) * DV] = jnp.sum(st_ref[b, h] * col, axis=0, keepdims=True)
    value_in.wait_recv()
    sums = total(uv, 4)
    scale = lax.rsqrt(sums[:, 1024:1025] / D + EPS)
    value = scale * sums[:, 0:1024]
    query = scale * query
    key = scale * key * DK ** (-0.5)
    kt[...] = jnp.transpose(key)
    rates, outs = [], []
    for h in range(HPD):
        head = jnp.full((1, 128), (tp * HPD + h).astype(F32), F32)
        rates.append((1.0 - jnp.exp2(-1.0 - 6.0 * head / (HEADS - 1)))[:, 0:1])
        keys = slice(h * DK, (h + 1) * DK)
        cols = slice(h * DV, (h + 1) * DV)
        qk = jnp.sum(query[:, keys] * key[:, keys], axis=1, keepdims=True)
        out = rates[h] * (scale * ret[:, cols]) + qk * value[:, cols]
        outs.append(out * lax.rsqrt(jnp.mean(out * out, axis=1, keepdims=True) + EPS))
    for h in range(HPD):
        gate_in[h].wait_recv()
        gate = scale * total(ug.at[h], 4)
        r4[h, kv] = (gate * jax.nn.sigmoid(gate) * outs[h]).astype(BF16)
        mixed_in.append(kv_gather(5 + h, r4.at[h]))

    ret[...] = value
    for b in range(ROWS):
        for h in range(HPD):
            col = kt[h * DK : (h + 1) * DK, b : b + 1]
            st_ref[b, h] = rates[h] * st_ref[b, h] + col * ret[b : b + 1, h * DV : (h + 1) * DV]

    local[5].wait()
    mixed_in[0].wait_recv()
    mixed = r4[0].astype(F32).reshape(128, DV).astype(BF16)
    tacc[...] = jnp.dot(mixed, wo[0:DV, :], preferred_element_type=F32).reshape(2, 64, 256)
    mixed_in[1].wait_recv()

    def half_terms(half):
        rows = r4[1, pl.ds(half * 8, 8)].astype(F32).reshape(64, DV).astype(BF16)
        return tacc[half] + jnp.dot(rows, wo[DV : 2 * DV, :], preferred_element_type=F32)

    mate = {"tp": pair}
    s5[...] = half_terms(1 - core).astype(BF16)
    remote(s5, rd, ts.at[2], tr.at[2], mate).start()
    kept = half_terms(core)
    step(tsem, 2, rd, mate).wait_recv()
    r5[chip] = (kept + rd[...].astype(F32)).astype(BF16)
    for d in (4, 2, 6):
        remote(r5.at[chip], r5.at[chip], ts.at[3], tr.at[3], {"tp": tpto[d]}).start()
    step(tsem, 3, r5.at[1:4], across).wait_recv()
    r6[core] = (xrows[core] + total(r5, 4)).astype(BF16)
    remote(r6.at[core], r6.at[core], ts.at[4], tr.at[4], mate).start()
    swapped = step(tsem, 4, r6.at[1 - core], mate)
    gains = jnp.concatenate(
        [sum(r1b[j, 32:48, :].astype(F32) for j in range(4 * i, 4 * i + 4)) for i in range(2)], axis=1
    )
    local[6].wait()

    def width(c):
        return UW + 128 if c == 0 else UW

    def up_half(half, chunks):
        rows = r6[half].astype(F32)
        cnormed = (rows * gains[0:1, :]).astype(BF16)
        mine = pl.ds(half * 8, 8)
        for c in chunks:
            if c == 0:
                msquares = jnp.sum(rows * rows, axis=1, keepdims=True)
                su[0, mine, :, UW : UW + 128] = jnp.broadcast_to(msquares, (64, 128)).reshape(8, ROWS, 128).astype(BF16)
            part = jnp.dot(cnormed, wu[:, c * UW : (c + 1) * UW], preferred_element_type=F32)
            su[c, mine, :, 0:UW] = part.reshape(8, ROWS, UW).astype(BF16)
            for d in (6, 2, 5, 3, 7, 1, 4, 0):
                peer = half * 8 + lax.rem(kv + d, 8)
                copy = remote(
                    su.at[c, peer, :, 0 : width(c)], ru.at[c, kv, :, 0 : width(c)],
                    ks.at[7 + c], kr.at[7 + c], {"kv": peer},
                )
                if d:
                    copy.start()
                else:
                    pl.when(peer != kv)(copy.start)

    early, late = range(NU // 2), range(NU // 2, NU)
    up_half(core, early)
    swapped.wait_recv()
    up_half(1 - core, early)
    middle = r6[...].astype(F32).reshape(128, 256)
    cnormed = (middle * gains[0:1, :]).astype(BF16)
    up_in, hidden_in = [], []
    for c in late:
        part = jnp.dot(cnormed, wu[:, c * UW : (c + 1) * UW], preferred_element_type=F32)
        su[c, :, :, 0:UW] = part.reshape(KV, ROWS, UW).astype(BF16)
        for o in PLANE:
            remote(
                su.at[c, to[o], :, 0:UW], ru.at[c, kv, :, 0:UW], ks.at[7 + c], kr.at[7 + c], {"kv": to[o]}
            ).start()
    for c in range(NU):
        ru[c, kv, :, 0 : width(c)] = su[c, kv, :, 0 : width(c)]
        up_in.append(step(ksem, 7 + c, ru.at[c, 1:KV, :, 0 : width(c)], aside))
    midt[...] = jnp.transpose(middle)
    for c in range(NU):
        up_in[c].wait_recv()
        if c == 0:
            up = total(ru.at[0], KV)
            cscale = lax.rsqrt(up[:, UW : UW + 1] / D + EPS)
            up = up[:, 0:UW]
        else:
            up = total(ru.at[c, :, :, 0:UW], KV)
        r7[c, kv] = jnp.square(jnp.maximum(cscale * up, 0.0)).astype(BF16)
        hidden_in.append(kv_gather(7 + NU + c, r7.at[c]))

    local[7].wait()
    down = jnp.zeros((128, 256), F32)
    for c in range(NU):
        hidden_in[c].wait_recv()
        hidden = r7[c].astype(F32).reshape(128, UW).astype(BF16)
        down = down + jnp.dot(hidden, wd[c * UW : (c + 1) * UW, :], preferred_element_type=F32)
    s8[...] = jnp.transpose(down).reshape(TP, 32, 128).astype(BF16)
    for d in (5, 4, 3, 6, 2, 7, 1):
        remote(s8.at[tpto[d]], r8.at[d], ts.at[5], tr.at[5], {"tp": tpto[d]}).start()
    r8[0] = s8[tp]
    step(tsem, 5, r8.at[1:TP], across).wait_recv()
    lowered = total(r8, TP)
    out_ref[...] = (midt[pl.ds(pl.multiple_of(tp * 32, 32), 32), :] + lowered).astype(BF16)
    for copy in sent:
        copy.wait_send()


def writer(a_ref, s_ref, out_ref, state_ref, sem):
    copies = [pltpu.make_async_copy(a_ref, out_ref, sem.at[ROWS])]
    copies += [pltpu.make_async_copy(s_ref.at[b], state_ref.at[b], sem.at[b]) for b in range(ROWS)]
    for c in copies:
        c.start()
    for c in copies:
        c.wait()


def per_device(x, mixer_gain, channel_gain, wq, wk, wv, wg, wo, wu, wd, state):
    vm = pl.BlockSpec(memory_space=pltpu.VMEM)
    hb = pl.BlockSpec(memory_space=pltpu.HBM)
    dma = pltpu.SemaphoreType.DMA
    v = lambda *shape: pltpu.VMEM(shape, BF16)
    f = lambda *shape: pltpu.VMEM(shape, F32)
    ringed = lambda n: (v(4, 4, ROWS, n), v(4, 4, ROWS, n), v(4, ROWS, n), v(4, ROWS, n))
    scratch = [
        v(256, 512), v(256, 512), v(256, 1024), v(256, 1024), v(1024, 256), v(256, 2048), v(2048, 256), v(2, 1, 32),
        v(32, 128), v(TP, 32, 128), v(48, 128), v(TP, 48, 128),
        *ringed(512), *ringed(512), *ringed(1152),
        v(HPD, 4, 4, ROWS, DV), v(HPD, 4, 4, ROWS, DV),
        v(HPD, 4, ROWS, DV), v(HPD, 4, ROWS, DV), v(HPD, KV, ROWS, DV), v(64, 256), v(64, 256), v(4, 64, 256), v(2, 64, 256),
        v(NU, KV, ROWS, UW + 128), v(NU, KV, ROWS, UW + 128), v(NU, KV, ROWS, UW),
        v(TP, 32, 128), v(TP, 32, 128),
        f(2, 64, 256), f(2, 64, 256), f(512, ROWS), f(512, ROWS), f(ROWS, 1024), f(256, 128),
        dma((11,)), dma((6,)), dma((6,)), dma((12 + 2 * NU,)), dma((12 + 2 * NU,)),
        pltpu.SemaphoreType.REGULAR,
    ]
    out, new_state = pl.pallas_call(
        kernel,
        name="layer",
        out_shape=(pltpu.VMEM((32, 128), BF16), pltpu.VMEM(state.shape, F32)),
        in_specs=[hb] * 11,
        out_specs=(vm, vm),
        scratch_shapes=scratch,
        compiler_params=pltpu.CompilerParams(
            collective_id=0, has_side_effects=True, vmem_limit_bytes=int(55.7 * 2**20)
        ),
    )(x.T, mixer_gain.reshape(1, 32), channel_gain.reshape(1, 32), wq, wk, wv, wg, wo, wu, wd, state)
    out, new_state = pl.pallas_call(
        writer,
        name="writer",
        out_shape=(jax.ShapeDtypeStruct((32, 128), BF16), jax.ShapeDtypeStruct(state.shape, F32)),
        in_specs=[vm, vm],
        out_specs=(hb, hb),
        scratch_shapes=[dma((ROWS + 1,))],
        compiler_params=pltpu.CompilerParams(vmem_limit_bytes=2**20),
    )(out, new_state)
    return out.T, new_state


def solution(mesh):
    return jax.shard_map(
        per_device,
        mesh=mesh,
        in_specs=(
            P(None, ("kv", "tp")),
            P(("kv", "tp")),
            P(("kv", "tp")),
            P("kv", "tp"),
            P("kv", "tp"),
            P("kv", "tp"),
            P("kv", "tp"),
            P("tp", "kv"),
            P("kv", "tp"),
            P("tp", "kv"),
            P("kv", "tp", None, None),
        ),
        out_specs=(P(None, ("kv", "tp")), P("kv", "tp", None, None)),
        check_vma=False,
    )
```

```python
import jax
import jax.numpy as jnp
from jax import lax
from jax.experimental import pallas as pl
from jax.experimental.pallas import tpu as pltpu
from jax.sharding import PartitionSpec as P

D = 4096
HEADS = 16
DK = 256
DV = 512
EPS = 1e-06
KV = 16
TP = 8
ROWS = 8
HPD = 2
NU = 4
UW = 2048 // NU
F32 = jnp.float32
BF16 = jnp.bfloat16
MESH = pl.DeviceIdType.MESH
HOPS = (0, 1, 2, 1)
PLANE = sorted(
    [(dz, dy) for dz in range(4) for dy in range(4) if dz or dy],
    key=lambda o: -(HOPS[o[0]] + HOPS[o[1]]),
)


def total(ref, n):
    acc = ref[0].astype(F32)
    for j in range(1, n):
        acc = acc + ref[j].astype(F32)
    return acc


def kernel(
    x_ref, mg_ref, cg_ref, wq_ref, wk_ref, wv_ref, wg_ref, wo_ref, wu_ref, wd_ref, state_ref,
    out_ref, st_ref,
    wq, wk, wv, wg, wo, wu, wd, gs,
    s1, r1, s1b, r1b, sq, rq, tq, uq, sk, rk, tk, uk, sv, rv, tv, uv, sg, rg, tg, ug, r4, s5, rd, r5, r6,
    su, ru, r7, s8, r8,
    xrows, tacc, qt, kt, ret, midt,
    lsem, ts, tr, ks, kr, plane,
):
    kv = lax.axis_index("kv")
    tp = lax.axis_index("tp")
    z, y = kv // 4, lax.rem(kv, 4)
    core, chip = lax.rem(tp, 2), tp // 2

    def plane_at(dz, dy):
        return lax.rem(z + dz, 4) * 4 + lax.rem(y + dy, 4)

    to = {o: plane_at(*o) for o in PLANE}
    tpto = [lax.rem(tp + d, TP) for d in range(TP)]
    pair = tp + 1 - 2 * core
    sent = []

    def remote(src, dst, send, recv, device):
        return pltpu.make_async_remote_copy(
            src_ref=src, dst_ref=dst, send_sem=send, recv_sem=recv,
            device_id=device, device_id_type=MESH,
        )

    def step(sems, i, slots, device):
        whole = remote(slots, slots, sems[0].at[i], sems[1].at[i], device)
        sent.append(whole)
        return whole

    ksem, tsem = (ks, kr), (ts, tr)
    aside, across = {"kv": to[0, 1]}, {"tp": tpto[1]}

    ring_at = {"z": (z, lambda q: {"kv": q * 4 + y}), "y": (y, lambda q: {"kv": z * 4 + q})}

    def ring_scatter(c, axis, s, r):
        me, device = ring_at[axis]
        part = (lambda q: s.at[q]) if axis == "z" else (lambda q: s.at[:, q])
        for d in (2, 1, 3):
            q = lax.rem(me + d, 4)
            remote(part(q), r.at[d], ks.at[c], kr.at[c], device(q)).start()
        r[0] = part(me)[...]
        return step(ksem, c, r.at[1:4], aside)

    def ring_finish(stage, c, axis, r, t, u):
        me, device = ring_at[axis]
        stage.wait_recv()
        t[...] = total(r, 4).astype(BF16)
        for d in (2, 1, 3):
            q = lax.rem(me + d, 4)
            remote(t.at[q], u.at[d], ks.at[c], kr.at[c], device(q)).start()
        u[0] = t[me]
        return step(ksem, c, u.at[1:4], aside)

    def kv_gather(c, r):
        for o in PLANE:
            remote(r.at[kv], r.at[kv], ks.at[c], kr.at[c], {"kv": to[o]}).start()
        return step(ksem, c, r.at[1:KV], aside)

    barrier = pltpu.get_barrier_semaphore()
    ring = [{"kv": to[o]} for o in PLANE if 0 in o]
    for device in ring + [{"tp": p} for p in tpto[1:]]:
        pl.semaphore_signal(barrier, inc=1, device_id=device, device_id_type=MESH)
    first = [
        pltpu.make_async_copy(x_ref, s1b.at[0:32], lsem.at[8]),
        pltpu.make_async_copy(mg_ref, gs.at[0], lsem.at[9]),
        pltpu.make_async_copy(cg_ref, gs.at[1], lsem.at[10]),
    ]
    local = [
        pltpu.make_async_copy(a, b, lsem.at[i])
        for i, (a, b) in enumerate(
            ((wq_ref, wq), (wk_ref, wk), (wv_ref, wv), (wg_ref, wg), (state_ref, st_ref),
             (wo_ref, wo), (wu_ref, wu), (wd_ref, wd))
        )
    ]
    for c in first + local[:4]:
        c.start()
    for c in first:
        c.wait()

    r32 = lax.broadcasted_iota(jnp.int32, (32, 32), 0)
    c32 = lax.broadcasted_iota(jnp.int32, (32, 32), 1)
    column = jnp.sum(jnp.where(r32 == c32, gs[0].astype(F32), 0.0), axis=1, keepdims=True)
    s1[...] = (s1b[0:32, :].astype(F32) * column).astype(BF16)
    r1[tp] = s1[...]
    place = lax.broadcasted_iota(jnp.int32, (32, 128), 0) + 32 * lax.rem(tp, 4)
    place = jnp.where(place == lax.broadcasted_iota(jnp.int32, (32, 128), 1), 1.0, 0.0).astype(BF16)
    row = lax.broadcasted_iota(jnp.int32, (16, 32), 0)
    both = jnp.where(row == 0, gs[1].astype(F32), 0.0).astype(BF16)
    s1b[32:48, :] = jnp.dot(both, place, preferred_element_type=F32).astype(BF16)
    r1b[tp] = s1b[...]
    pl.semaphore_wait(barrier, len(ring) + TP - 1)

    for d in (5, 4, 3, 6, 2, 7, 1):
        remote(s1, r1.at[tp], ts.at[0], tr.at[0], {"tp": tpto[d]}).start()
    for d in (5, 4, 3, 6, 2, 7, 1):
        remote(s1b, r1b.at[tp], ts.at[1], tr.at[1], {"tp": tpto[d]}).start()
    first_in = step(tsem, 0, r1.at[1:TP], across)
    second_in = step(tsem, 1, r1b.at[1:TP], across)
    for c in local[4:]:
        c.start()
    for o in PLANE:
        if o[1] == 0:
            pl.semaphore_signal(plane, inc=1, device_id={"kv": to[o]}, device_id_type=MESH)
    first_in.wait_recv()
    normed = jnp.transpose(r1[...].astype(F32).reshape(256, 128)).astype(BF16)

    local[0].wait()
    sq[...] = jnp.dot(normed, wq[...], preferred_element_type=F32).reshape(4, 4, ROWS, 512).astype(BF16)
    pl.semaphore_wait(plane, 3)
    query_in = ring_scatter(0, "z", sq, rq)
    local[1].wait()
    sk[...] = jnp.dot(normed, wk[...], preferred_element_type=F32).reshape(4, 4, ROWS, 512).astype(BF16)
    key_in = ring_scatter(1, "z", sk, rk)
    second_in.wait_recv()
    x = jnp.transpose(jnp.concatenate([r1b[j, 0:32, :].astype(F32) for j in range(TP)], axis=0))
    xrows[...] = x.reshape(2, 64, 256)
    squares = jnp.sum(x * x, axis=1, keepdims=True)
    local[2].wait()
    sv[:, :, :, 0:1024] = jnp.dot(normed, wv[...], preferred_element_type=F32).reshape(4, 4, ROWS, 1024).astype(BF16)
    sv[:, :, :, 1024:1152] = jnp.broadcast_to(squares, (128, 128)).reshape(4, 4, ROWS, 128).astype(BF16)
    value_in = ring_scatter(2, "y", sv, rv)
    local[3].wait()
    gate_in, mixed_in = [], []
    for h in range(HPD):
        part = jnp.dot(normed, wg[:, h * DV : (h + 1) * DV], preferred_element_type=F32)
        sg[h] = part.reshape(4, 4, ROWS, DV).astype(BF16)
        gate_in.append(ring_scatter(3 + h, "zy"[h], sg.at[h], rg.at[h]))

    query_in = ring_finish(query_in, 7 + 2 * NU, "y", rq, tq, uq)
    key_in = ring_finish(key_in, 7 + 2 * NU + 1, "y", rk, tk, uk)
    value_in = ring_finish(value_in, 7 + 2 * NU + 2, "z", rv, tv, uv)
    for h in range(HPD):
        gate_in[h] = ring_finish(gate_in[h], 10 + 2 * NU + h, "yz"[h], rg.at[h], tg.at[h], ug.at[h])
    query_in.wait_recv()
    query = total(uq, 4)
    qt[...] = jnp.transpose(query)
    key_in.wait_recv()
    key = total(uk, 4)
    local[4].wait()
    for b in range(ROWS):
        for h in range(HPD):
            col = qt[h * DK : (h + 1) * DK, b : b + 1]
            ret[b : b + 1, h * DV : (h + 1) * DV] = jnp.sum(st_ref[b, h] * col, axis=0, keepdims=True)
    value_in.wait_recv()
    sums = total(uv, 4)
    scale = lax.rsqrt(sums[:, 1024:1025] / D + EPS)
    value = scale * sums[:, 0:1024]
    query = scale * query
    key = scale * key * DK ** (-0.5)
    kt[...] = jnp.transpose(key)
    rates, outs = [], []
    for h in range(HPD):
        head = jnp.full((1, 128), (tp * HPD + h).astype(F32), F32)
        rates.append((1.0 - jnp.exp2(-1.0 - 6.0 * head / (HEADS - 1)))[:, 0:1])
        keys = slice(h * DK, (h + 1) * DK)
        cols = slice(h * DV, (h + 1) * DV)
        qk = jnp.sum(query[:, keys] * key[:, keys], axis=1, keepdims=True)
        out = rates[h] * (scale * ret[:, cols]) + qk * value[:, cols]
        outs.append(out * lax.rsqrt(jnp.mean(out * out, axis=1, keepdims=True) + EPS))
    for h in range(HPD):
        gate_in[h].wait_recv()
        gate = scale * total(ug.at[h], 4)
        r4[h, kv] = (gate * jax.nn.sigmoid(gate) * outs[h]).astype(BF16)
        mixed_in.append(kv_gather(5 + h, r4.at[h]))

    ret[...] = value
    for b in range(ROWS):

        @pl.loop(0, HPD)
        def _(h):
            col = kt[pl.ds(h * DK, DK), b : b + 1]
            rate = jnp.where(h == 0, rates[0], rates[1])
            st_ref[b, h] = rate * st_ref[b, h] + col * ret[b : b + 1, pl.ds(pl.multiple_of(h * DV, DV), DV)]

    local[5].wait()
    mixed_in[0].wait_recv()
    mixed = r4[0].astype(F32).reshape(128, DV).astype(BF16)
    tacc[...] = jnp.dot(mixed, wo[0:DV, :], preferred_element_type=F32).reshape(2, 64, 256)
    mixed_in[1].wait_recv()

    def half_terms(half):
        rows = r4[1, pl.ds(half * 8, 8)].astype(F32).reshape(64, DV).astype(BF16)
        return tacc[half] + jnp.dot(rows, wo[DV : 2 * DV, :], preferred_element_type=F32)

    mate = {"tp": pair}
    s5[...] = half_terms(1 - core).astype(BF16)
    remote(s5, rd, ts.at[2], tr.at[2], mate).start()
    kept = half_terms(core)
    step(tsem, 2, rd, mate).wait_recv()
    r5[chip] = (kept + rd[...].astype(F32)).astype(BF16)
    for d in (4, 2, 6):
        remote(r5.at[chip], r5.at[chip], ts.at[3], tr.at[3], {"tp": tpto[d]}).start()
    step(tsem, 3, r5.at[1:4], across).wait_recv()
    r6[core] = (xrows[core] + total(r5, 4)).astype(BF16)
    remote(r6.at[core], r6.at[core], ts.at[4], tr.at[4], mate).start()
    swapped = step(tsem, 4, r6.at[1 - core], mate)
    gains = jnp.concatenate(
        [sum(r1b[j, 32:48, :].astype(F32) for j in range(4 * i, 4 * i + 4)) for i in range(2)], axis=1
    )
    local[6].wait()

    def width(c):
        return UW + 128 if c == 0 else UW

    def up_half(half, chunks):
        rows = r6[half].astype(F32)
        cnormed = (rows * gains[0:1, :]).astype(BF16)
        mine = pl.ds(half * 8, 8)
        for c in chunks:
            if c == 0:
                msquares = jnp.sum(rows * rows, axis=1, keepdims=True)
                su[0, mine, :, UW : UW + 128] = jnp.broadcast_to(msquares, (64, 128)).reshape(8, ROWS, 128).astype(BF16)
            part = jnp.dot(cnormed, wu[:, c * UW : (c + 1) * UW], preferred_element_type=F32)
            su[c, mine, :, 0:UW] = part.reshape(8, ROWS, UW).astype(BF16)
            for d in (6, 2, 5, 3, 7, 1, 4, 0):
                peer = half * 8 + lax.rem(kv + d, 8)
                copy = remote(
                    su.at[c, peer, :, 0 : width(c)], ru.at[c, kv, :, 0 : width(c)],
                    ks.at[7 + c], kr.at[7 + c], {"kv": peer},
                )
                if d:
                    copy.start()
                else:
                    pl.when(peer != kv)(copy.start)

    early, late = range(NU // 2), range(NU // 2, NU)
    up_half(core, early)
    swapped.wait_recv()
    up_half(1 - core, early)
    middle = r6[...].astype(F32).reshape(128, 256)
    cnormed = (middle * gains[0:1, :]).astype(BF16)
    up_in, hidden_in = [], []
    for c in late:
        part = jnp.dot(cnormed, wu[:, c * UW : (c + 1) * UW], preferred_element_type=F32)
        su[c, :, :, 0:UW] = part.reshape(KV, ROWS, UW).astype(BF16)
        for o in PLANE:
            remote(
                su.at[c, to[o], :, 0:UW], ru.at[c, kv, :, 0:UW], ks.at[7 + c], kr.at[7 + c], {"kv": to[o]}
            ).start()
    for c in range(NU):
        ru[c, kv, :, 0 : width(c)] = su[c, kv, :, 0 : width(c)]
        up_in.append(step(ksem, 7 + c, ru.at[c, 1:KV, :, 0 : width(c)], aside))
    midt[...] = jnp.transpose(middle)
    for c in range(NU):
        up_in[c].wait_recv()
        if c == 0:
            up = total(ru.at[0], KV)
            cscale = lax.rsqrt(up[:, UW : UW + 1] / D + EPS)
            up = up[:, 0:UW]
        else:
            up = total(ru.at[c, :, :, 0:UW], KV)
        r7[c, kv] = jnp.square(jnp.maximum(cscale * up, 0.0)).astype(BF16)
        hidden_in.append(kv_gather(7 + NU + c, r7.at[c]))

    local[7].wait()
    down = jnp.zeros((128, 256), F32)
    for c in range(NU):
        hidden_in[c].wait_recv()
        hidden = r7[c].astype(F32).reshape(128, UW).astype(BF16)
        down = down + jnp.dot(hidden, wd[c * UW : (c + 1) * UW, :], preferred_element_type=F32)
    s8[...] = jnp.transpose(down).reshape(TP, 32, 128).astype(BF16)
    for d in (5, 4, 3, 6, 2, 7, 1):
        remote(s8.at[tpto[d]], r8.at[d], ts.at[5], tr.at[5], {"tp": tpto[d]}).start()
    r8[0] = s8[tp]
    step(tsem, 5, r8.at[1:TP], across).wait_recv()
    lowered = total(r8, TP)
    out_ref[...] = (midt[pl.ds(pl.multiple_of(tp * 32, 32), 32), :] + lowered).astype(BF16)
    for copy in sent:
        copy.wait_send()


def writer(a_ref, s_ref, out_ref, state_ref, sem):
    copies = [pltpu.make_async_copy(a_ref, out_ref, sem.at[ROWS])]
    copies += [pltpu.make_async_copy(s_ref.at[b], state_ref.at[b], sem.at[b]) for b in range(ROWS)]
    for c in copies:
        c.start()
    for c in copies:
        c.wait()


def per_device(x, mixer_gain, channel_gain, wq, wk, wv, wg, wo, wu, wd, state):
    vm = pl.BlockSpec(memory_space=pltpu.VMEM)
    hb = pl.BlockSpec(memory_space=pltpu.HBM)
    dma = pltpu.SemaphoreType.DMA
    v = lambda *shape: pltpu.VMEM(shape, BF16)
    f = lambda *shape: pltpu.VMEM(shape, F32)
    ringed = lambda n: (v(4, 4, ROWS, n), v(4, 4, ROWS, n), v(4, ROWS, n), v(4, ROWS, n))
    scratch = [
        v(256, 512), v(256, 512), v(256, 1024), v(256, 1024), v(1024, 256), v(256, 2048), v(2048, 256), v(2, 1, 32),
        v(32, 128), v(TP, 32, 128), v(48, 128), v(TP, 48, 128),
        *ringed(512), *ringed(512), *ringed(1152),
        v(HPD, 4, 4, ROWS, DV), v(HPD, 4, 4, ROWS, DV),
        v(HPD, 4, ROWS, DV), v(HPD, 4, ROWS, DV), v(HPD, KV, ROWS, DV), v(64, 256), v(64, 256), v(4, 64, 256), v(2, 64, 256),
        v(NU, KV, ROWS, UW + 128), v(NU, KV, ROWS, UW + 128), v(NU, KV, ROWS, UW),
        v(TP, 32, 128), v(TP, 32, 128),
        f(2, 64, 256), f(2, 64, 256), f(512, ROWS), f(512, ROWS), f(ROWS, 1024), f(256, 128),
        dma((11,)), dma((6,)), dma((6,)), dma((12 + 2 * NU,)), dma((12 + 2 * NU,)),
        pltpu.SemaphoreType.REGULAR,
    ]
    out, new_state = pl.pallas_call(
        kernel,
        name="layer",
        out_shape=(pltpu.VMEM((32, 128), BF16), pltpu.VMEM(state.shape, F32)),
        in_specs=[hb] * 11,
        out_specs=(vm, vm),
        scratch_shapes=scratch,
        compiler_params=pltpu.CompilerParams(
            collective_id=0, has_side_effects=True, vmem_limit_bytes=int(55.7 * 2**20)
        ),
    )(x.T, mixer_gain.reshape(1, 32), channel_gain.reshape(1, 32), wq, wk, wv, wg, wo, wu, wd, state)
    out, new_state = pl.pallas_call(
        writer,
        name="writer",
        out_shape=(jax.ShapeDtypeStruct((32, 128), BF16), jax.ShapeDtypeStruct(state.shape, F32)),
        in_specs=[vm, vm],
        out_specs=(hb, hb),
        scratch_shapes=[dma((ROWS + 1,))],
        compiler_params=pltpu.CompilerParams(vmem_limit_bytes=2**20),
    )(out, new_state)
    return out.T, new_state


def solution(mesh):
    return jax.shard_map(
        per_device,
        mesh=mesh,
        in_specs=(
            P(None, ("kv", "tp")),
            P(("kv", "tp")),
            P(("kv", "tp")),
            P("kv", "tp"),
            P("kv", "tp"),
            P("kv", "tp"),
            P("kv", "tp"),
            P("tp", "kv"),
            P("kv", "tp"),
            P("tp", "kv"),
            P("kv", "tp", None, None),
        ),
        out_specs=(P(None, ("kv", "tp")), P("kv", "tp", None, None)),
        check_vma=False,
    )
```
